256 devices in a mesh: grp: 2 (over y), fs: 16 (over z), tp: 8 (over x, core).
Axes of the slice: x: 4, y: 2, z: 16, core: 2. Of those that a mesh axis runs over, the one named last changes fastest.
The devices are a block of a 4x16x16 slice.
Arguments:
- tokens: bfloat16 [32768, 2048], P(('grp', 'fs', 'tp')), parts along dimension 0, may hold values from -6 to 6
- first_gain: float32 [2048], replicated, may hold values from 0.1 to 1.9
- mixer_gain: float32 [2048], replicated, may hold values from 0.1 to 1.9
- gate_weight: bfloat16 [2048, 4608], P('fs', 'tp'), may hold values from -0.125 to 0.125
- up_weight: bfloat16 [2048, 4608], P('fs', 'tp'), may hold values from -0.125 to 0.125
- down_weight: bfloat16 [4608, 2048], P('tp', 'fs'), may hold values from -0.09375 to 0.09375
- query_weight: bfloat16 [2048, 2048], P('fs', 'tp'), may hold values from -0.125 to 0.125
- key_weight: bfloat16 [2048, 2048], P('fs', 'tp'), may hold values from -0.125 to 0.125
- value_weight: bfloat16 [2048, 4096], P('fs', 'tp'), may hold values from -0.125 to 0.125
- head_gain: float32 [4096], P('tp'), may hold values from 0.1 to 1.9
- out_weight: bfloat16 [4096, 2048], P('tp', 'fs'), may hold values from -0.09375 to 0.09375
- log_decay: float32 [2, 8], P(None, 'tp'), may hold values from -0.03125 to 0, as said below
Outputs:
- updated: bfloat16 [32768, 2048], P(('grp', 'fs', 'tp')), parts along dimension 0
The draws below stay inside these ranges and needn't reach their ends.
There are 2 independent parts, one for each index of `grp`. The reference program is written for one: setup_inputs(seed, part) draws one part's arguments, and reference() takes and returns one part's arrays. A program takes and returns all parts, laid end to end along the dimension named above; an argument that names none is the same for every part. Nothing has to cross between parts.
Inputs may be any that keep to these rules, and one draw needn't show every extreme that they name: `log_decay`: log decay per step of each direction (forward, then backward) and head.
All inputs are finite; a program needn't handle non-finite values.
Results may differ from the reference program's by a relative error of at most 0.02.
Values may be sent and summed in bfloat16 or wider, within the bound.
A program may use at most 64 MiB of HBM per device.

```python
import math
import jax
import jax.numpy as jnp
from jax import lax

D = 2048
H = 8
DK = 256
DV = 512
FF = 4608
BLOCK = 128
TOK = 1024
TOKENS = 16384
N_TP = 8


def draw_log_decay(key, part):
    order = jax.random.permutation(jax.random.fold_in(key, 11), H)
    fast_count = H // 2
    fast_heads = order < fast_count
    unit = jax.random.uniform(jax.random.fold_in(key, 12), (2, H), jnp.float32)
    slow_rate = math.log(0.1) / TOK * (0.1 + 0.9 * unit)
    fast_rate = -4.0 / BLOCK + unit * (4.0 / BLOCK - 4.0 / (3.0 * BLOCK))
    return jnp.where(fast_heads[None, :], fast_rate, slow_rate).astype(jnp.float32)


def block_scale(stream_key, shape, cuts, smallest, top_value):
    level, own = 1.0, jax.random.fold_in(stream_key, 6)
    for position, parts in cuts:
        heights = jnp.exp(jax.random.uniform(jax.random.fold_in(own, position), (parts,), jnp.float32, smallest / len(cuts), top_value / len(cuts)))
        level = level * jnp.repeat(heights, shape[position] // parts).reshape([-1 if axis == position else 1 for axis in range(len(shape))])
    return level


def centred(own_key, dims, scale, limit, cuts=(), held_as=jnp.bfloat16):
    level = block_scale(own_key, dims, cuts, -0.22, 0.18) if cuts else 1.0
    drawn = jax.random.normal(own_key, dims, jnp.float32) * scale * level
    return jnp.minimum(jnp.maximum(drawn, -limit), limit).astype(held_as)


def setup_inputs(seed: int = 0, part: int = 0) -> dict:
    arg_keys = jax.random.split(jax.random.key(seed), 13)
    part_splits = jax.random.split(jax.random.fold_in(arg_keys[12], part), 13)
    tokens = centred(part_splits[0], (TOKENS, D), 1.0, 6.0, ((0, 128),))
    first_gain = jnp.clip(1.0 + 0.18 * jax.random.normal(arg_keys[1], (D,), jnp.float32), 0.1, 1.9)
    mixer_gain = jnp.clip(1.0 + 0.18 * jax.random.normal(arg_keys[2], (D,), jnp.float32), 0.1, 1.9)
    gate_weight = centred(arg_keys[3], (D, FF), D ** -0.5, 0.125, ((0, 16), (1, 8)))
    up_weight = centred(arg_keys[4], (D, FF), D ** -0.5, 0.125, ((0, 16), (1, 8)))
    down_weight = centred(arg_keys[5], (FF, D), FF ** -0.5, 0.09375, ((0, 8), (1, 16)))
    query_weight = centred(arg_keys[6], (D, H * DK), D ** -0.5, 0.125, ((0, 16), (1, 8)))
    key_weight = centred(arg_keys[7], (D, H * DK), D ** -0.5, 0.125, ((0, 16), (1, 8)))
    value_weight = centred(arg_keys[8], (D, H * DV), D ** -0.5, 0.125, ((0, 16), (1, 8)))
    head_gain = jnp.clip(1.0 + 0.18 * jax.random.normal(arg_keys[9], (H * DV,), jnp.float32), 0.1, 1.9)
    out_weight = centred(arg_keys[10], (H * DV, D), (H * DV) ** -0.5, 0.09375, ((0, 8), (1, 16)))
    log_decay = draw_log_decay(jax.random.fold_in(arg_keys[12], 71), part)
    return {"tokens": tokens, "first_gain": first_gain, "mixer_gain": mixer_gain, "gate_weight": gate_weight, "up_weight": up_weight, "down_weight": down_weight, "query_weight": query_weight, "key_weight": key_weight, "value_weight": value_weight, "head_gain": head_gain, "out_weight": out_weight, "log_decay": log_decay}


EPS = 1e-06

def norm_rows(values, gain):
    widened = values.astype(jnp.float32)
    factor = lax.rsqrt(lax.optimization_barrier(jnp.mean(widened * widened, axis=-1, keepdims=True)) + EPS)
    return (widened * factor * gain).astype(jnp.bfloat16)

def split_sum(left, right, pieces):
    width = left.shape[1] // pieces
    running = jnp.zeros((left.shape[0], right.shape[1]), jnp.float32)
    for which_block in range(pieces):
        product = jnp.dot(left[:, which_block * width:(which_block + 1) * width], right[which_block * width:(which_block + 1) * width], preferred_element_type=jnp.float32)
        running = running + lax.optimization_barrier(product.astype(jnp.bfloat16)).astype(jnp.float32)
    return running

def sweep_one(queries, key_rows, value_rows, log_rate):
    length = queries.shape[0]
    block_count = length // BLOCK
    places = jnp.arange(BLOCK, dtype=jnp.float32)
    distance = places[:, None] - places[None, :]
    inner_decay = jnp.where(distance >= 0, jnp.exp(log_rate * jnp.maximum(distance, 0.0)), 0.0)
    enter_decay = jnp.exp(log_rate * (places + 1.0))
    leave_decay = jnp.exp(log_rate * (BLOCK - 1.0 - places))
    block_decay = jnp.exp(log_rate * BLOCK)
    highest = lax.Precision.HIGHEST

    def advance(memory, blocks):
        query_block, key_block, value_block = blocks
        scores = jnp.dot(query_block.astype(jnp.bfloat16), key_block.astype(jnp.bfloat16).T, preferred_element_type=jnp.float32) * inner_decay
        result = jnp.dot(scores, value_block, precision=highest)
        result = result + jnp.dot(query_block, memory, precision=highest) * enter_decay[:, None]
        memory = memory * block_decay + jnp.dot((key_block * leave_decay[:, None]).T, value_block, precision=highest)
        return (memory, result)
    start_memory = jnp.zeros((queries.shape[1], value_rows.shape[1]), jnp.float32)
    _, results = lax.scan(advance, start_memory, (queries.reshape(block_count, BLOCK, -1), key_rows.reshape(block_count, BLOCK, -1), value_rows.reshape(block_count, BLOCK, -1)))
    return results.reshape(length, -1)

def retain_both(queries, key_rows, value_rows, forward_rate, backward_rate):
    forward_part = sweep_one(queries, key_rows, value_rows, forward_rate)
    backward_part = sweep_one(jnp.flip(queries, axis=0), jnp.flip(key_rows, axis=0), jnp.flip(value_rows, axis=0), backward_rate)
    return forward_part + jnp.flip(backward_part, axis=0)

def head_norm(outputs, gain):
    heads_here = gain.shape[0] // DV
    centered = outputs - lax.optimization_barrier(jnp.mean(outputs, axis=-1, keepdims=True))
    variance = lax.optimization_barrier(jnp.mean(centered * centered, axis=-1, keepdims=True))
    return centered * lax.rsqrt(variance + EPS) * gain.reshape(heads_here, 1, DV)

def feed_half(residual, gain, gate_weight, up_weight, down_weight):
    normed = norm_rows(residual, gain)
    gate_sum = jnp.dot(normed, gate_weight, preferred_element_type=jnp.float32)
    up_sum = jnp.dot(normed, up_weight, preferred_element_type=jnp.float32)
    hidden = (jax.nn.silu(gate_sum) * up_sum).astype(jnp.bfloat16)
    branch = split_sum(hidden, down_weight, N_TP)
    return (residual.astype(jnp.float32) + 0.5 * branch).astype(jnp.bfloat16)

def to_heads(values, width):
    widened = lax.optimization_barrier(values.astype(jnp.bfloat16)).astype(jnp.float32)
    return widened.reshape(-1, TOK, H, width).transpose(0, 2, 1, 3)

def mix_tokens(residual, gain, query_weight, key_weight, value_weight, head_gain, out_weight, log_decay):
    normed = norm_rows(residual, gain)
    queries = to_heads(jnp.dot(normed, query_weight, preferred_element_type=jnp.float32), DK) * DK ** (-0.5)
    key_rows = to_heads(jnp.dot(normed, key_weight, preferred_element_type=jnp.float32), DK)
    value_rows = to_heads(jnp.dot(normed, value_weight, preferred_element_type=jnp.float32), DV)

    def per_sequence(blocks):
        return jax.vmap(retain_both)(blocks[0], blocks[1], blocks[2], log_decay[0], log_decay[1])
    outputs = lax.map(per_sequence, (queries, key_rows, value_rows))
    normed_heads = head_norm(outputs, head_gain).astype(jnp.bfloat16)
    flat = normed_heads.transpose(0, 2, 1, 3).reshape(-1, H * DV)
    branch = split_sum(flat, out_weight, N_TP)
    return (residual.astype(jnp.float32) + branch).astype(jnp.bfloat16)

def reference(tokens, first_gain, mixer_gain, gate_weight, up_weight, down_weight, query_weight, key_weight, value_weight, head_gain, out_weight, log_decay):
    after_first = feed_half(tokens, first_gain, gate_weight, up_weight, down_weight)
    return mix_tokens(after_first, mixer_gain, query_weight, key_weight, value_weight, head_gain, out_weight, log_decay)
```

```python
import functools

import jax
import jax.numpy as jnp
from jax import lax
from jax.experimental import pallas as pl
from jax.experimental.pallas import tpu as pltpu
from jax.sharding import PartitionSpec as P

EPS = 1e-06
MESH = pl.DeviceIdType.MESH
F32, BF16 = jnp.float32, jnp.bfloat16
LANES = 128
ROW_TILE = 16
STEP_TILE = 512
PAIR_SHARE = (0.25, 0.34, 0.375, 0.3125)


def split_rows(rows, share):
    pair = int(rows * share) // ROW_TILE * ROW_TILE
    first = -(-(rows - pair) // (2 * ROW_TILE)) * ROW_TILE
    return first, rows - pair - first, pair


def half_mask(tile):
    return lax.broadcasted_iota(jnp.int32, tile.shape, 1) < LANES // 2


def kernel(
    sizes,
    tok_in,
    gain1,
    gain2,
    gate_in,
    up_in,
    down_in,
    q_in,
    k_in,
    v_in,
    hgain,
    out_in,
    rates,
    o_ref,
    gu,
    dn,
    qkv,
    wo,
    x1,
    x1n,
    acc,
    hid,
    p1,
    r1,
    s1,
    h1,
    f1,
    x2,
    p2,
    r2,
    s2,
    h2,
    f2,
    qs,
    ks,
    vs,
    decay,
    hn,
    ss,
    z_send,
    z_recv,
    y_send,
    y_recv,
    x_send,
    x_recv,
    a_send,
    a_recv,
    local_sem,
):
    n, groups = sizes
    half = n // 2
    d = n * LANES
    me = lax.axis_index("fs")
    r = lax.axis_index("tp")
    g = lax.axis_index("grp")
    up_z, down_z = lax.rem(me + 1, n), lax.rem(me + n - 1, n)
    x, c = r // 2, lax.rem(r, 2)
    xr, xl, xo = lax.rem(x + 1, 4), lax.rem(x + 3, 4), lax.rem(x + 2, 4)
    r_right, r_left, r_far = xr * 2 + c, xl * 2 + c, xo * 2 + c
    r_mate = x * 2 + 1 - c
    odd = lax.rem(g, 2)
    g_mate = g + 1 - 2 * odd
    rows = x1.shape[1]
    ff = gate_in.shape[1]
    main = ff // LANES * LANES
    tail = ff - main
    started = []

    def remote(src, dst, ss_, rs_, **to):
        return pltpu.make_async_remote_copy(
            src_ref=src, dst_ref=dst, send_sem=ss_, recv_sem=rs_, device_id=to, device_id_type=MESH
        )

    def send(ref, dst, ss_, rs_, **to):
        copy = remote(ref, dst, ss_, rs_, **to)
        copy.start()
        started.append(copy)

    def arrived(ref, ss_, rs_, **to):
        remote(ref, ref, ss_, rs_, **to).wait_recv()

    local = []

    def fetch(src, dst):
        copy = pltpu.make_async_copy(src, dst, local_sem.at[len(local)])
        copy.start()
        local.append(copy)

    fetch(tok_in, x1.at[r])
    fetch(down_in, dn.at[me, pl.ds(0, ff)])
    dk, dv = q_in.shape[1], v_in.shape[1]
    fetch(q_in, qkv.at[me, :, pl.ds(0, dk)])
    fetch(k_in, qkv.at[me, :, pl.ds(dk, dk)])
    fetch(v_in, qkv.at[me, :, pl.ds(2 * dk, dv)])
    fetch(out_in, wo.at[me])

    gu[me, :, :main] = gate_in[:, :main]
    gu[me, :, main : 2 * main] = up_in[:, :main]
    gu[me, :, 2 * main :] = jnp.concatenate([gate_in[:, main:], up_in[:, main:]], axis=1)

    barrier = pltpu.get_barrier_semaphore()
    neighbours = [
        {"fs": up_z},
        {"fs": down_z},
        {"tp": r_right},
        {"tp": r_left},
        {"tp": r_mate},
        {"grp": g_mate},
    ]
    for to in neighbours:
        pl.semaphore_signal(barrier, inc=1, device_id=to, device_id_type=MESH)
    pl.semaphore_wait(barrier, len(neighbours))
    for copy in local:
        copy.wait()

    kinds = (gu, dn, qkv, wo)
    lengths = (gu.shape[1], ff, qkv.shape[1], wo.shape[1])
    parts = [split_rows(length, share) for length, share in zip(lengths, PAIR_SHARE)]

    def z_rows(kind, sub):
        first, second, pair = parts[kind]
        if sub == 0:
            return pl.ds(pl.multiple_of(odd * (lengths[kind] - first), ROW_TILE), first)
        return pl.ds(pl.multiple_of(first + odd * (pair - first), ROW_TILE), second)

    def y_rows(kind, sent):
        pair = parts[kind][2]
        at = odd if sent else 1 - odd
        return pl.ds(pl.multiple_of(at * (lengths[kind] - pair), ROW_TILE), pair)

    def before(s):
        return lax.rem(me + n - s, n)

    def after(s):
        return lax.rem(me + s, n)

    def hops(sub, way):
        return half if sub == way else half - 1

    def z_start(kind, sub, way, s):
        block = before(s) if way == 0 else after(s)
        ref = kinds[kind].at[block, z_rows(kind, sub)]
        slot = (2 * kind + sub, way, s)
        send(ref, ref, z_send.at[slot], z_recv.at[slot], fs=up_z if way == 0 else down_z)

    def z_event(kind, sub, s):
        for way in range(2):
            if s > hops(sub, way):
                continue
            block = before(s) if way == 0 else after(s)
            ref = kinds[kind].at[block, z_rows(kind, sub)]
            slot = (2 * kind + sub, way, s - 1)
            arrived(ref, z_send.at[slot], z_recv.at[slot], fs=down_z if way == 0 else up_z)
            if s < hops(sub, way):
                z_start(kind, sub, way, s)
            if sub == 0:
                ref = kinds[kind].at[block, y_rows(kind, True)]
                slot = (kind, way, s - 1)
                send(ref, ref, y_send.at[slot], y_recv.at[slot], grp=g_mate)

    def y_wait(kind, s):
        for way in range(2):
            if s > hops(0, way):
                continue
            block = before(s) if way == 0 else after(s)
            ref = kinds[kind].at[block, y_rows(kind, False)]
            slot = (kind, way, s - 1)
            arrived(ref, y_send.at[slot], y_recv.at[slot], grp=g_mate)

    def pair_of(s):
        return (before(s), after(s)) if s < half else (me, after(half))

    def gather_start(buf, k):
        ref = buf(r)
        for i, to in enumerate((r_right, r_left, r_mate)):
            send(ref, ref, a_send.at[k, i], a_recv.at[k, i], tp=to)

    def gather_on(buf, k, count):
        for i, (src, onward) in enumerate(((r_left, r_right), (r_right, r_left))):
            ref = buf(src)
            arrived(ref, a_send.at[k, i], a_recv.at[k, i], tp=src)
            part = buf(src, pl.ds(i * (count // 2), count // 2))
            send(part, part, a_send.at[k, 3 + i], a_recv.at[k, 3 + i], tp=onward)
            send(ref, ref, a_send.at[k, 5 + i], a_recv.at[k, 5 + i], tp=r_mate)

    def gather_far(buf, k, count):
        for i, src in enumerate((r_left, r_right)):
            part = buf(r_far, pl.ds(i * (count // 2), count // 2))
            arrived(part, a_send.at[k, 3 + i], a_recv.at[k, 3 + i], tp=src)
        ref = buf(r_far)
        send(ref, ref, a_send.at[k, 7], a_recv.at[k, 7], tp=r_mate)

    def gather_mate(buf, k):
        for i, src in ((2, x), (5, xl), (6, xr), (7, xo)):
            ref = buf(src * 2 + 1 - c)
            arrived(ref, a_send.at[k, i], a_recv.at[k, i], tp=r_mate)

    def x1_buf(block, part=None):
        return x1.at[block] if part is None else x1.at[block, part]

    def x2_buf(q):
        def buf(block, part=None):
            return x2.at[q, block] if part is None else x2.at[q, block, part]

        return buf

    def sum_start(phase, q):
        p_, r_ = (p1, r1) if phase == 0 else (p2, r2)
        send(p_.at[q, 1 - c], r_.at[q], x_send.at[phase, q, 0], x_recv.at[phase, q, 0], tp=r_mate)

    def sum_chip(phase, q):
        p_, r_, s_, h_ = (p1, r1, s1, h1) if phase == 0 else (p2, r2, s2, h2)
        arrived(r_.at[q], x_send.at[phase, q, 0], x_recv.at[phase, q, 0], tp=r_mate)

        def add(to):
            s_[q, to] = (p_[q, c, to].astype(F32) + r_[q, to].astype(F32)).astype(BF16)

        add(xo)
        for i, to in enumerate((r_right, r_left)):
            part = pl.ds(i * (rows // 2), rows // 2)
            send(s_.at[q, xo, part], h_.at[q, i], x_send.at[phase, q, 1 + i], x_recv.at[phase, q, 1 + i], tp=to)
        add(xr)
        add(xl)
        add(x)

    def sum_on(phase, q):
        s_, h_, f_ = (s1, h1, f1) if phase == 0 else (s2, h2, f2)
        for i, (src, to, x_to) in enumerate(((r_left, r_right, xr), (r_right, r_left, xl))):
            arrived(h_.at[q, i], x_send.at[phase, q, 1 + i], x_recv.at[phase, q, 1 + i], tp=src)
            part = pl.ds(i * (rows // 2), rows // 2)
            s_[q, x_to, part] = (s_[q, x_to, part].astype(F32) + h_[q, i].astype(F32)).astype(BF16)
            send(s_.at[q, x_to], f_.at[q, i], x_send.at[phase, q, 3 + i], x_recv.at[phase, q, 3 + i], tp=to)

    def sum_end(phase, q):
        s_, f_ = (s1, f1) if phase == 0 else (s2, f2)
        for i, src in enumerate((r_left, r_right)):
            arrived(f_.at[q, i], x_send.at[phase, q, 3 + i], x_recv.at[phase, q, 3 + i], tp=src)
        return s_[q, x].astype(F32) + f_[q, 0].astype(F32) + f_[q, 1].astype(F32)

    def block_lanes(block):
        return pl.ds(pl.multiple_of(block * LANES, LANES), LANES)

    def blocks_of(q):
        per = STEP_TILE // LANES // 2
        return [b for s in range(q * per + 1, (q + 1) * per + 1) for b in pair_of(s)]

    def after_first(q):
        total = sum_end(0, q)
        for i, block in enumerate(blocks_of(q)):
            cols = slice(i * LANES, (i + 1) * LANES)
            base = x1[r, :, block_lanes(block)].astype(F32)
            x2[q, r, :, cols] = (base + 0.5 * total[:, cols]).astype(BF16)
        gather_start(x2_buf(q), 1 + q)

    def updated(q):
        total = sum_end(1, q) + x2[q, r].astype(F32)
        for i, block in enumerate(blocks_of(q)):
            o_ref[:, block_lanes(block)] = total[:, i * LANES : (i + 1) * LANES].astype(BF16)

    seq = x1n.shape[1]
    tile = seq // 2

    def norm_tokens(first, last):
        def body(i, carry):
            value = x1[i].astype(F32)
            factor = lax.rsqrt(jnp.mean(value * value, axis=1, keepdims=True) + EPS)
            value = (value * factor * gain1[...]).astype(BF16)
            to = pl.ds(pl.multiple_of(i * rows, rows), rows)
            for b in range(n):
                x1n[b, to] = value[:, b * LANES : (b + 1) * LANES]
            return carry

        lax.fori_loop(first, last, body, 0)

    def tiles(step, count=2):
        def body(m, carry):
            step(m)
            return carry

        lax.fori_loop(0, count, body, 0)

    def gu_compute(s):
        y_wait(0, s)
        a, b = pair_of(s)

        def step(m):
            part = pl.ds(pl.multiple_of(m * tile, tile), tile)
            left = jnp.concatenate([x1n[a, part], x1n[b, part]], axis=1)
            right = jnp.concatenate([gu[a], gu[b]], axis=0)
            product = jnp.dot(left, right, preferred_element_type=F32)
            acc[part] = product if s == 1 else acc[part] + product

        tiles(step)

    def silu_times(gate, up_value):
        return gate / (1.0 + jnp.exp(-gate)) * up_value

    def hidden():
        size = seq // 8

        def step(m):
            part = pl.ds(pl.multiple_of(m * size, size), size)
            hid[part, :main] = silu_times(acc[part, :main], acc[part, main : 2 * main]).astype(BF16)
            last = acc[part, 2 * main :]
            value = silu_times(last, pltpu.roll(last, LANES // 2, 1))
            hid[part, main:] = jnp.where(half_mask(value), value, 0.0).astype(BF16)

        tiles(step, 8)

    def project(kind, s, left, p_):
        y_wait(kind, s)
        a, b = pair_of(s)
        w = kinds[kind]
        q, at = (s - 1) // 2, (s - 1) % 2 * 2 * LANES

        def step(m):
            part = pl.ds(pl.multiple_of(m * tile, tile), tile)
            right = jnp.concatenate([w[a], w[b]], axis=1)
            product = jnp.dot(left[part], right, preferred_element_type=F32).astype(BF16)
            for i in range(tile // rows):
                to = m * (tile // rows // 2) + i // 2
                p_[q, i % 2, to, :, at : at + 2 * LANES] = product[i * rows : (i + 1) * rows]

        tiles(step)

    def qkv_compute(s):
        y_wait(2, s)
        a, b = pair_of(s)
        q, at = (s - 1) // 2, (s - 1) % 2 * 2 * LANES
        gain = jnp.concatenate([gain2[:, block_lanes(a)], gain2[:, block_lanes(b)]], axis=1)
        per = tile // rows
        width = qkv.shape[2]

        def step(m):
            part = pl.ds(pl.multiple_of(m * tile, tile), tile)
            value = x2[q, pl.ds(m * per, per), :, at : at + 2 * LANES].reshape(tile, 2 * LANES).astype(F32)
            square = value * value
            square = square[:, :LANES] + square[:, LANES:]
            right = jnp.concatenate([qkv[a], qkv[b]], axis=0)
            product = jnp.dot((value * gain).astype(BF16), right, preferred_element_type=F32)
            acc[part, :width] = product if s == 1 else acc[part, :width] + product
            ss[part] = square if s == 1 else ss[part] + square

        tiles(step)

    def qkv_end():
        size = seq // 4
        scale = dk**-0.5

        def step(m):
            part = pl.ds(pl.multiple_of(m * size, size), size)
            factor = lax.rsqrt(jnp.sum(ss[part], axis=1, keepdims=True) / d + EPS)
            qs[part] = ((acc[part, :dk] * factor).astype(BF16).astype(F32) * scale).astype(BF16)
            ks[part] = (acc[part, dk : 2 * dk] * factor).astype(BF16)
            vs[part] = (acc[part, 2 * dk : 2 * dk + dv] * factor).astype(BF16)

        tiles(step, 4)

    def make_decay(first, last):
        size = seq // 8
        forward, backward = rates[0, 0], rates[1, 0]

        def body(m, carry):
            at = lax.broadcasted_iota(jnp.int32, (size, seq), 0) + m * size
            gap = at - lax.broadcasted_iota(jnp.int32, (size, seq), 1)
            far = gap.astype(F32)
            weight = jnp.exp(jnp.where(gap >= 0, forward * far, -backward * far))
            decay[pl.ds(pl.multiple_of(m * size, size), size)] = jnp.where(gap == 0, 2.0, weight)
            return carry

        lax.fori_loop(first, last, body, 0)

    def retention():
        size = seq // 4

        def step(m):
            part = pl.ds(pl.multiple_of(m * size, size), size)
            score = lax.dot_general(qs[part], ks[...], (((1,), (1,)), ((), ())), preferred_element_type=F32)
            kept = jnp.dot((score * decay[part]).astype(BF16), vs[...], preferred_element_type=F32)
            kept = kept - jnp.mean(kept, axis=1, keepdims=True)
            variance = jnp.mean(kept * kept, axis=1, keepdims=True)
            hn[part] = (kept * lax.rsqrt(variance + EPS) * hgain[...]).astype(BF16)

        tiles(step, 4)

    def clear_padding():
        pad = dn.shape[1] - ff

        def body(i, carry):
            dn[i, ff:] = jnp.zeros((pad, LANES), BF16)
            return carry

        if pad:
            lax.fori_loop(0, n, body, 0)

    plan = []

    def at(place, what, *args):
        plan.append((place, len(plan), functools.partial(what, *args)))

    def ring_starts(place, kind, sub):
        for way in range(2):
            at(place, z_start, kind, sub, way, 0)

    place = {}
    order = [(0, sub, s) for s in range(1, half + 1) for sub in range(2)]
    for s in range(1, half + 1):
        order += [(1, 0, s), (2, 0, s), (1, 1, s)]
    lag = 3
    for slot in range(1, half + 1 + lag):
        if slot <= half:
            order.append((2, 1, slot))
        if slot > lag:
            order += [(3, 0, slot - lag), (3, 1, slot - lag)]
    for i, event in enumerate(order):
        place[event] = i
        at(i, z_event, *event)
    for kind in range(4):
        for sub in range(2):
            ring_starts(-1 if kind == 0 else place[kind, sub, 1] - 2.5, kind, sub)

    at(-0.9, gather_start, x1_buf, 0)
    at(-0.5, clear_padding)
    for i in range(4):
        at(0.5 + i, make_decay, 2 * i, 2 * i + 2)
    at(4.5, gather_on, x1_buf, 0, rows)
    at(6.5, gather_far, x1_buf, 0, rows)
    at(7.5, gather_mate, x1_buf, 0)
    at(7.6, norm_tokens, 0, 4)
    at(8.6, norm_tokens, 4, 8)
    when = 9.5
    for s in range(1, half + 1):
        when = max(when + 0.5, place[0, 1, s] + 1.5)
        at(when, gu_compute, s)
    at(when + 0.1, hidden)
    when += 0.2
    chunks = d // STEP_TILE
    per = half // chunks
    gathered = []
    for q in range(chunks):
        for s in range(q * per + 1, (q + 1) * per + 1):
            when = max(when + 0.5, place[1, 1, s] + 1.5)
            at(when, project, 1, s, hid, p1)
        at(when + 0.1, sum_start, 0, q)
        at(when + 2.2, sum_chip, 0, q)
        at(when + 5.2, sum_on, 0, q)
        at(when + 8.2, after_first, q)
        at(when + 11.2, gather_on, x2_buf(q), 1 + q, rows)
        at(when + 13.2, gather_far, x2_buf(q), 1 + q, rows)
        at(when + 14.2, gather_mate, x2_buf(q), 1 + q)
        gathered.append(when + 14.2)
    when = 0
    for s in range(1, half + 1):
        when = max(when + 0.5, place[2, 1, s] + 1.5, gathered[(s - 1) // per] + 0.1)
        at(when, qkv_compute, s)
    at(when + 0.1, qkv_end)
    at(when + 0.2, retention)
    when += 0.3
    for q in range(chunks):
        for s in range(q * per + 1, (q + 1) * per + 1):
            when = max(when + 0.5, place[3, 1, s] + 1.5)
            at(when, project, 3, s, hn, p2)
        at(when + 0.1, sum_start, 1, q)
        at(when + 1.2, sum_chip, 1, q)
        at(when + 2.2, sum_on, 1, q)
        at(when + 3.2, updated, q)

    for _, _, what in sorted(plan, key=lambda entry: entry[:2]):
        what()
    for copy in started:
        copy.wait_send()


def solution(mesh):
    n, n_tp, groups = mesh.shape["fs"], mesh.shape["tp"], mesh.shape["grp"]

    def shards(tokens, g1, g2, gate, up, down, query, key, value, head_gain, out, log_decay):
        rows, d = tokens.shape
        ff = gate.shape[1]
        dk, dv = query.shape[1], value.shape[1]
        seq = rows * n_tp
        chunks = d // STEP_TILE
        ff_pad = -(-ff // LANES) * LANES
        vmem = pl.BlockSpec(memory_space=pltpu.VMEM)
        hbm = pl.BlockSpec(memory_space=pl.ANY)
        sums = [
            pltpu.VMEM((chunks, 2, n_tp // 2, rows, STEP_TILE), BF16),
            pltpu.VMEM((chunks, n_tp // 2, rows, STEP_TILE), BF16),
            pltpu.VMEM((chunks, n_tp // 2, rows, STEP_TILE), BF16),
            pltpu.VMEM((chunks, 2, rows // 2, STEP_TILE), BF16),
            pltpu.VMEM((chunks, 2, rows, STEP_TILE), BF16),
        ]
        dma = pltpu.SemaphoreType.DMA
        return pl.pallas_call(
            functools.partial(kernel, (n, groups)),
            out_shape=jax.ShapeDtypeStruct((rows, d), BF16),
            in_specs=[hbm, vmem, vmem, vmem, vmem, hbm, hbm, hbm, hbm, vmem, hbm, pl.BlockSpec(memory_space=pltpu.SMEM)],
            out_specs=vmem,
            scratch_shapes=[
                pltpu.VMEM((n, LANES, 2 * ff), BF16),
                pltpu.VMEM((n, ff_pad, LANES), BF16),
                pltpu.VMEM((n, LANES, 2 * dk + dv), BF16),
                pltpu.VMEM((n, dv, LANES), BF16),
                pltpu.VMEM((n_tp, rows, d), BF16),
                pltpu.VMEM((n, seq, LANES), BF16),
                pltpu.VMEM((seq, 2 * ff), F32),
                pltpu.VMEM((seq, ff_pad), BF16),
                *sums,
                pltpu.VMEM((chunks, n_tp, rows, STEP_TILE), BF16),
                *sums,
                pltpu.VMEM((seq, dk), BF16),
                pltpu.VMEM((seq, dk), BF16),
                pltpu.VMEM((seq, dv), BF16),
                pltpu.VMEM((seq, seq), F32),
                pltpu.VMEM((seq, dv), BF16),
                pltpu.VMEM((seq, LANES), F32),
                dma((8, 2, n // 2)),
                dma((8, 2, n // 2)),
                dma((4, 2, n // 2)),
                dma((4, 2, n // 2)),
                dma((2, chunks, 5)),
                dma((2, chunks, 5)),
                dma((1 + chunks, 8)),
                dma((1 + chunks, 8)),
                dma((6,)),
            ],
            compiler_params=pltpu.CompilerParams(
                collective_id=0, has_side_effects=True, vmem_limit_bytes=67_000_000
            ),
        )(
            tokens,
            g1.reshape(1, -1),
            g2.reshape(1, -1),
            gate,
            up,
            down,
            query,
            key,
            value,
            head_gain.reshape(1, -1),
            out,
            log_decay,
        )

    placed = (
        P(("grp", "fs", "tp"), None),
        P(),
        P(),
        P("fs", "tp"),
        P("fs", "tp"),
        P("tp", "fs"),
        P("fs", "tp"),
        P("fs", "tp"),
        P("fs", "tp"),
        P("tp"),
        P("tp", "fs"),
        P(None, "tp"),
    )
    return jax.shard_map(
        shards, mesh=mesh, in_specs=placed, out_specs=P(("grp", "fs", "tp"), None), check_vma=False
    )
```

```python
import functools

import jax
import jax.numpy as jnp
from jax import lax
from jax.experimental import pallas as pl
from jax.experimental.pallas import tpu as pltpu
from jax.sharding import PartitionSpec as P

EPS = 1e-06
MESH = pl.DeviceIdType.MESH
F32, BF16 = jnp.float32, jnp.bfloat16
LANES = 128
ROW_TILE = 16
STEP_TILE = 256
SHORTER = ((0, 1), (1, 0), (0, 1), (0, 1))
PAIR_SHARE = (0.36, 0.43, 0.36, 0.36)
RING_STARTS = ((((0, 0, 4),), ((0, 0, 6),)), (((1, 1, 2),), ((1, 1, 3),)), (((2, 0, 5),), ((1, 1, 8),)))
RANKS = {}
GU_TIME = 1.07
LINK, MATE = 46650.0, 600000.0
LATENCY = {"z0": 2.0, "z1": 2.0, "x0": 2.0, "x1": 2.0, "m": 1.1, "y": 2.0}


def split_rows(rows, share):
    pair = int(rows * share) // ROW_TILE * ROW_TILE
    first = max(-(-(rows - pair) // (2 * ROW_TILE)) * ROW_TILE, pair)
    return first, rows - pair - first, pair


def actions(sizes):
    half, parts, row_bytes, hops = (sizes[k] for k in ("half", "parts", "row_bytes", "hops"))
    per, chunk = sizes["per"], sizes["chunk_bytes"]
    lasts = [per * (q + 1) for q in range(half // per)]
    acts = {}

    def act(name, rank, time, after=(), need=(), sends=()):
        acts[name] = (RANKS.get(name[0], rank), time, list(after), list(need), list(sends))

    def ways(kind, s):
        return [w for w in range(2) if s <= hops[kind][w]]

    def over_pair(kind, s):
        return [("y", kind, w, s) for w in ways(kind, s)]

    for kind in range(4):
        nbytes = [rows * row_bytes[kind] for rows in parts[kind]]
        for sub in range(2):
            after = [("z_event", *v) for v in RING_STARTS[kind - 1][sub]] if kind else []
            own = [(f"z{w}", nbytes[sub], ("z", kind, sub, w, 1)) for w in range(2)]
            act(("z_own", kind, sub), -10 + 0.1 * kind, 0.03, after, (), own)
            for s in range(1, half + 1):
                need = [("z", kind, sub, w, s) for w in ways(kind, s)]
                onward = [(f"z{w}", nbytes[sub], ("z", kind, sub, w, s + 1)) for w in ways(kind, s + 1)]
                after = [("z_event", kind, sub, s - 1) if s > 1 else ("z_own", kind, sub)]
                act(("z_event", kind, sub, s), -20 + kind, 0.05, after, need, onward)
        for s in range(1, half + 1):
            after = [("z_event", kind, 0, s)]
            if s > 1 or kind:
                after.append(("y_start", kind, s - 1) if s > 1 else ("y_start", kind - 1, half))
            act(("y_start", kind, s), -15 + kind, 0.02, after, (), [("y", nbytes[2], v) for v in over_pair(kind, s)])

    def gather(k, nbytes, first, rank):
        on = [("x0", nbytes / 2, 3), ("m", nbytes, 5), ("x1", nbytes / 2, 4), ("m", nbytes, 6)]
        for name, time, after, need, sends in (
            ("gather_on", 0.05, first, (0, 1), on),
            ("gather_far", 0.03, ("gather_on", k), (3, 4), [("m", nbytes, 7)]),
            ("gather_mate", 0.01, ("gather_far", k), (2, 5, 6, 7), []),
        ):
            tags = [("g", k, i) for i in need]
            act((name, k), rank, time, [after], tags, [(a, b, ("g", k, i)) for a, b, i in sends])
        return [(to, nbytes, ("g", k, i)) for i, to in enumerate(("x0", "x1", "m"))]

    sends = gather(0, sizes["tok_bytes"], ("gather_start", 0), -5)
    act(("gather_start", 0), -30, 0.06, (), (), sends)
    act(("clear_padding",), 50, 0.09)
    decays = [("make_decay", 2 * i, 2 * i + 2) for i in range(4)]
    for name in decays:
        act(name, 60, 0.36)
    norms = [("norm_tokens", 0, 4), ("norm_tokens", 4, 8)]
    for name in norms:
        act(name, -3, 0.92, [("gather_mate", 0)])
    for s in range(1, half + 1):
        after = [("z_event", 0, sub, s) for sub in range(2)] + (norms if s == 1 else [("gu_compute", s - 1)])
        act(("gu_compute", s), 0, GU_TIME, after, over_pair(0, s))
    act(("hidden",), 0, 0.85, [("gu_compute", half)])
    for phase in range(2):
        kind = 3 if phase else 1
        first = ("retention",) if phase else ("hidden",)
        for s in range(1, half + 1):
            after = [("z_event", kind, sub, s) for sub in range(2)] + [("project", phase, s - 1) if s > 1 else first]
            act(("project", phase, s), 1 + phase, 0.6 if phase else 0.75, after + [("clear_padding",)], over_pair(kind, s))
        for q in range(len(lasts)):
            tag = [("s", phase, q, i) for i in range(5)]
            act(("sum_start", phase, q), -4, 0.02, [("project", phase, lasts[q])], (), [("m", 4 * chunk, tag[0])])
            sends = [("x0", chunk / 2, tag[1]), ("x1", chunk / 2, tag[2])]
            act(("sum_chip", phase, q), -5, 0.16, [("sum_start", phase, q)], tag[:1], sends)
            sends = [("x0", chunk, tag[3]), ("x1", chunk, tag[4])]
            act(("sum_on", phase, q), -6, 0.06, [("sum_chip", phase, q)], tag[1:3], sends)
            after = [("sum_on", phase, q)]
            if phase:
                act(("updated", q), -1, 0.2, after, tag[3:])
            else:
                sends = gather(1 + q, chunk, ("after_first", q), -8)
                act(("after_first", q), -7, 0.14, after, tag[3:], sends)
    for s in range(1, half + 1):
        after = [("gather_mate", 1 + min(q for q, last in enumerate(lasts) if s <= last)), ("z_event", 2, 0, s), ("z_event", 2, 1, s)]
        after.append(("qkv_compute", s - 1) if s > 1 else ("hidden",))
        act(("qkv_compute", s), 1.5, 0.92, after, over_pair(2, s))
    act(("qkv_end",), 0, 0.67, [("qkv_compute", half)])
    act(("retention",), 0, 3.1, [("qkv_end",)] + decays)
    return acts


def in_order(acts, trace=None):
    arrival, free, done, left, now = {}, {}, set(), dict(acts), 0.0
    while left:
        ready = []
        for place, (name, (rank, _, after, need, _)) in enumerate(left.items()):
            if all(v in done for v in after) and all(v in arrival for v in need):
                ready.append((max([now] + [arrival[v] for v in need]), rank, place, name))
        begin, _, _, name = min(ready)
        _, time, _, _, sends = left.pop(name)
        if trace is not None:
            trace.append((name, now, begin))
        now = begin + time
        done.add(name)
        for link, nbytes, tag in sends:
            free[link] = max(free.get(link, 0.0), now) + nbytes / (MATE if link == "m" else LINK)
            arrival[tag] = free[link] + LATENCY[link]
        yield name


def half_mask(tile):
    return lax.broadcasted_iota(jnp.int32, tile.shape, 1) < LANES // 2


def kernel(
    sizes,
    tok_in,
    gain1,
    gain2,
    gate_in,
    up_in,
    down_in,
    q_in,
    k_in,
    v_in,
    hgain,
    out_in,
    rates,
    o_ref,
    gu,
    dn,
    qkv,
    wo,
    x1,
    x1n,
    acc,
    hid,
    p1,
    r1,
    s1,
    h1,
    f1,
    x2,
    p2,
    r2,
    s2,
    h2,
    f2,
    qs,
    ks,
    vs,
    decay,
    hn,
    ss,
    z_send,
    z_recv,
    y_send,
    y_recv,
    x_send,
    x_recv,
    a_send,
    a_recv,
    local_sem,
):
    n, groups = sizes
    half = n // 2
    d = n * LANES
    me = lax.axis_index("fs")
    r = lax.axis_index("tp")
    g = lax.axis_index("grp")
    up_z, down_z = lax.rem(me + 1, n), lax.rem(me + n - 1, n)
    x, c = r // 2, lax.rem(r, 2)
    xr, xl, xo = lax.rem(x + 1, 4), lax.rem(x + 3, 4), lax.rem(x + 2, 4)
    r_right, r_left, r_far = xr * 2 + c, xl * 2 + c, xo * 2 + c
    r_mate = x * 2 + 1 - c
    odd = lax.rem(g, 2)
    g_mate = g + 1 - 2 * odd
    rows = x1.shape[1]
    ff = gate_in.shape[0]
    main = ff // LANES * LANES
    started = []
    per = STEP_TILE // LANES // 2

    def remote(src, dst, ss_, rs_, **to):
        return pltpu.make_async_remote_copy(
            src_ref=src, dst_ref=dst, send_sem=ss_, recv_sem=rs_, device_id=to, device_id_type=MESH
        )

    def send(ref, dst, ss_, rs_, **to):
        copy = remote(ref, dst, ss_, rs_, **to)
        copy.start()
        started.append(copy)

    def arrived(ref, ss_, rs_, **to):
        remote(ref, ref, ss_, rs_, **to).wait_recv()

    local = []

    def fetch(src, dst):
        copy = pltpu.make_async_copy(src, dst, local_sem.at[len(local)])
        copy.start()
        local.append(copy)

    for i, weight in enumerate((gate_in, up_in)):
        fetch(weight.at[pl.ds(0, main)], gu.at[me, pl.ds(i * main, main)])
        fetch(weight.at[pl.ds(main, ff - main)], gu.at[me, pl.ds(2 * main + i * (ff - main), ff - main)])
    fetch(tok_in, x1.at[r])
    fetch(down_in, dn.at[me, pl.ds(0, ff)])
    dk, dv = q_in.shape[1], v_in.shape[1]
    fetch(q_in, qkv.at[me, :, pl.ds(0, dk)])
    fetch(k_in, qkv.at[me, :, pl.ds(dk, dk)])
    fetch(v_in, qkv.at[me, :, pl.ds(2 * dk, dv)])
    fetch(out_in, wo.at[me])

    barrier = pltpu.get_barrier_semaphore()
    neighbours = [
        {"fs": up_z},
        {"fs": down_z},
        {"tp": r_right},
        {"tp": r_left},
        {"tp": r_mate},
        {"grp": g_mate},
    ]
    for to in neighbours:
        pl.semaphore_signal(barrier, inc=1, device_id=to, device_id_type=MESH)
    with jax.named_scope("entry"):
        pl.semaphore_wait(barrier, len(neighbours))
    with jax.named_scope("fetched"):
        for copy in local:
            copy.wait()

    kinds = (gu, dn, qkv, wo)
    lengths = (gu.shape[1], ff, qkv.shape[1], wo.shape[1])
    parts = [split_rows(length, share) for length, share in zip(lengths, PAIR_SHARE)]

    def z_rows(kind, sub):
        first, second, pair = parts[kind]
        if sub == 0:
            return pl.ds(pl.multiple_of(odd * (lengths[kind] - first), ROW_TILE), first)
        return pl.ds(pl.multiple_of(first + odd * (pair - first), ROW_TILE), second)

    def y_rows(kind, sent):
        pair = parts[kind][2]
        at = odd if sent else 1 - odd
        return pl.ds(pl.multiple_of(at * (lengths[kind] - pair), ROW_TILE), pair)

    def before(s):
        return lax.rem(me + n - s, n)

    def after(s):
        return lax.rem(me + s, n)

    def hops(kind, way):
        return half - SHORTER[kind][way]

    def z_start(kind, sub, way, s):
        block = before(s) if way == 0 else after(s)
        ref = kinds[kind].at[block, z_rows(kind, sub)]
        slot = (2 * kind + sub, way, s)
        send(ref, ref, z_send.at[slot], z_recv.at[slot], fs=up_z if way == 0 else down_z)

    def z_event(kind, sub, s):
        for way in range(2):
            if s > hops(kind, way):
                continue
            block = before(s) if way == 0 else after(s)
            ref = kinds[kind].at[block, z_rows(kind, sub)]
            slot = (2 * kind + sub, way, s - 1)
            arrived(ref, z_send.at[slot], z_recv.at[slot], fs=down_z if way == 0 else up_z)
            if s < hops(kind, way):
                z_start(kind, sub, way, s)
    def y_start(kind, s):
        for way in range(2):
            if s > hops(kind, way):
                continue
            block = before(s) if way == 0 else after(s)
            ref = kinds[kind].at[block, y_rows(kind, True)]
            slot = (kind, way, s - 1)
            send(ref, ref, y_send.at[slot], y_recv.at[slot], grp=g_mate)

    def z_own(kind, sub):
        for way in range(2):
            z_start(kind, sub, way, 0)

    def y_wait(kind, s):
        for way in range(2):
            if s > hops(kind, way):
                continue
            block = before(s) if way == 0 else after(s)
            ref = kinds[kind].at[block, y_rows(kind, False)]
            slot = (kind, way, s - 1)
            arrived(ref, y_send.at[slot], y_recv.at[slot], grp=g_mate)

    def pair_of(s):
        return (before(s), after(s)) if s < half else (me, after(half))

    def gather_start(buf, k):
        ref = buf(r)
        for i, to in enumerate((r_right, r_left, r_mate)):
            send(ref, ref, a_send.at[k, i], a_recv.at[k, i], tp=to)

    def gather_on(buf, k, count):
        for i, (src, onward) in enumerate(((r_left, r_right), (r_right, r_left))):
            ref = buf(src)
            arrived(ref, a_send.at[k, i], a_recv.at[k, i], tp=src)
            part = buf(src, pl.ds(i * (count // 2), count // 2))
            send(part, part, a_send.at[k, 3 + i], a_recv.at[k, 3 + i], tp=onward)
            send(ref, ref, a_send.at[k, 5 + i], a_recv.at[k, 5 + i], tp=r_mate)

    def gather_far(buf, k, count):
        for i, src in enumerate((r_left, r_right)):
            part = buf(r_far, pl.ds(i * (count // 2), count // 2))
            arrived(part, a_send.at[k, 3 + i], a_recv.at[k, 3 + i], tp=src)
        ref = buf(r_far)
        send(ref, ref, a_send.at[k, 7], a_recv.at[k, 7], tp=r_mate)

    def gather_mate(buf, k):
        for i, src in ((2, x), (5, xl), (6, xr), (7, xo)):
            ref = buf(src * 2 + 1 - c)
            arrived(ref, a_send.at[k, i], a_recv.at[k, i], tp=r_mate)

    def x1_buf(block, part=None):
        return x1.at[block] if part is None else x1.at[block, part]

    def x2_buf(q):
        def buf(block, part=None):
            return x2.at[q, block] if part is None else x2.at[q, block, part]

        return buf

    def sum_start(phase, q):
        p_, r_ = (p1, r1) if phase == 0 else (p2, r2)
        send(p_.at[q, 1 - c], r_.at[q], x_send.at[phase, q, 0], x_recv.at[phase, q, 0], tp=r_mate)

    def sum_chip(phase, q):
        p_, r_, s_, h_ = (p1, r1, s1, h1) if phase == 0 else (p2, r2, s2, h2)
        arrived(r_.at[q], x_send.at[phase, q, 0], x_recv.at[phase, q, 0], tp=r_mate)

        def add(to):
            s_[q, to] = (p_[q, c, to].astype(F32) + r_[q, to].astype(F32)).astype(BF16)

        add(xo)
        for i, to in enumerate((r_right, r_left)):
            part = pl.ds(i * (rows // 2), rows // 2)
            send(s_.at[q, xo, part], h_.at[q, i], x_send.at[phase, q, 1 + i], x_recv.at[phase, q, 1 + i], tp=to)
        add(xr)
        add(xl)
        add(x)

    def sum_on(phase, q):
        s_, h_, f_ = (s1, h1, f1) if phase == 0 else (s2, h2, f2)
        for i, (src, to, x_to) in enumerate(((r_left, r_right, xr), (r_right, r_left, xl))):
            arrived(h_.at[q, i], x_send.at[phase, q, 1 + i], x_recv.at[phase, q, 1 + i], tp=src)
            part = pl.ds(i * (rows // 2), rows // 2)
            s_[q, x_to, part] = (s_[q, x_to, part].astype(F32) + h_[q, i].astype(F32)).astype(BF16)
            send(s_.at[q, x_to], f_.at[q, i], x_send.at[phase, q, 3 + i], x_recv.at[phase, q, 3 + i], tp=to)

    def sum_end(phase, q):
        s_, f_ = (s1, f1) if phase == 0 else (s2, f2)
        for i, src in enumerate((r_left, r_right)):
            arrived(f_.at[q, i], x_send.at[phase, q, 3 + i], x_recv.at[phase, q, 3 + i], tp=src)
        return s_[q, x].astype(F32) + f_[q, 0].astype(F32) + f_[q, 1].astype(F32)

    def block_lanes(block):
        return pl.ds(pl.multiple_of(block * LANES, LANES), LANES)

    def blocks_of(q):
        return [b for s in range(q * per + 1, (q + 1) * per + 1) for b in pair_of(s)]

    def after_first(q):
        total = sum_end(0, q)
        for i, block in enumerate(blocks_of(q)):
            cols = slice(i * LANES, (i + 1) * LANES)
            base = x1[r, :, block_lanes(block)].astype(F32)
            x2[q, r, :, cols] = (base + 0.5 * total[:, cols]).astype(BF16)
        gather_start(x2_buf(q), 1 + q)

    def updated(q):
        total = sum_end(1, q) + x2[q, r].astype(F32)
        for i, block in enumerate(blocks_of(q)):
            o_ref[:, block_lanes(block)] = total[:, i * LANES : (i + 1) * LANES].astype(BF16)

    seq = x1n.shape[1]
    tile = seq // 2

    def norm_tokens(first, last):
        def body(i, carry):
            value = x1[i].astype(F32)
            factor = lax.rsqrt(jnp.mean(value * value, axis=1, keepdims=True) + EPS)
            value = (value * factor * gain1[...]).astype(BF16)
            to = pl.ds(pl.multiple_of(i * rows, rows), rows)
            for b in range(n):
                x1n[b, to] = value[:, b * LANES : (b + 1) * LANES]
            return carry

        lax.fori_loop(first, last, body, 0)

    def tiles(step, count=2):
        def body(m, carry):
            step(m)
            return carry

        lax.fori_loop(0, count, body, 0)

    def gu_compute(s):
        y_wait(0, s)
        a, b = pair_of(s)

        def step(m):
            part = pl.ds(pl.multiple_of(m * tile, tile), tile)
            left = jnp.concatenate([x1n[a, part], x1n[b, part]], axis=1)
            right = jnp.concatenate([gu[a], gu[b]], axis=1)
            product = lax.dot_general(left, right, (((1,), (1,)), ((), ())), preferred_element_type=F32)
            acc[part] = product if s == 1 else acc[part] + product

        tiles(step)

    def silu_times(gate, up_value):
        return gate / (1.0 + jnp.exp(-gate)) * up_value

    def hidden():
        size = seq // 8

        def step(m):
            part = pl.ds(pl.multiple_of(m * size, size), size)
            hid[part, :main] = silu_times(acc[part, :main], acc[part, main : 2 * main]).astype(BF16)
            last = acc[part, 2 * main :]
            value = silu_times(last, pltpu.roll(last, LANES // 2, 1))
            hid[part, main:] = jnp.where(half_mask(value), value, 0.0).astype(BF16)

        tiles(step, 8)

    def project(kind, s, left, p_):
        y_wait(kind, s)
        a, b = pair_of(s)
        w = kinds[kind]
        q, at = (s - 1) // per, (s - 1) % per * 2 * LANES

        def step(m):
            part = pl.ds(pl.multiple_of(m * tile, tile), tile)
            right = jnp.concatenate([w[a], w[b]], axis=1)
            product = jnp.dot(left[part], right, preferred_element_type=F32).astype(BF16)
            for i in range(tile // rows):
                to = m * (tile // rows // 2) + i // 2
                p_[q, i % 2, to, :, at : at + 2 * LANES] = product[i * rows : (i + 1) * rows]

        tiles(step)

    def qkv_compute(s):
        y_wait(2, s)
        a, b = pair_of(s)
        q, at = (s - 1) // per, (s - 1) % per * 2 * LANES
        gain = jnp.concatenate([gain2[:, block_lanes(a)], gain2[:, block_lanes(b)]], axis=1)
        count = tile // rows
        width = qkv.shape[2]

        def step(m):
            part = pl.ds(pl.multiple_of(m * tile, tile), tile)
            value = x2[q, pl.ds(m * count, count), :, at : at + 2 * LANES].reshape(tile, 2 * LANES).astype(F32)
            square = value * value
            square = square[:, :LANES] + square[:, LANES:]
            right = jnp.concatenate([qkv[a], qkv[b]], axis=0)
            product = jnp.dot((value * gain).astype(BF16), right, preferred_element_type=F32)
            acc[part, :width] = product if s == 1 else acc[part, :width] + product
            ss[part] = square if s == 1 else ss[part] + square

        tiles(step)

    def qkv_end():
        size = seq // 4
        scale = dk**-0.5

        def step(m):
            part = pl.ds(pl.multiple_of(m * size, size), size)
            factor = lax.rsqrt(jnp.sum(ss[part], axis=1, keepdims=True) / d + EPS)
            qs[part] = ((acc[part, :dk] * factor).astype(BF16).astype(F32) * scale).astype(BF16)
            ks[part] = (acc[part, dk : 2 * dk] * factor).astype(BF16)
            vs[part] = (acc[part, 2 * dk : 2 * dk + dv] * factor).astype(BF16)

        tiles(step, 4)

    def make_decay(first, last):
        size = seq // 8
        forward, backward = rates[0, 0], rates[0, 1]

        def body(m, carry):
            at = lax.broadcasted_iota(jnp.int32, (size, seq), 0) + m * size
            gap = at - lax.broadcasted_iota(jnp.int32, (size, seq), 1)
            far = gap.astype(F32)
            weight = jnp.exp(jnp.where(gap >= 0, forward * far, -backward * far))
            decay[pl.ds(pl.multiple_of(m * size, size), size)] = jnp.where(gap == 0, 2.0, weight)
            return carry

        lax.fori_loop(first, last, body, 0)

    def retention():
        size = seq // 4

        def step(m):
            part = pl.ds(pl.multiple_of(m * size, size), size)
            score = lax.dot_general(qs[part], ks[...], (((1,), (1,)), ((), ())), preferred_element_type=F32)
            kept = jnp.dot((score * decay[part]).astype(BF16), vs[...], preferred_element_type=F32)
            kept = kept - jnp.mean(kept, axis=1, keepdims=True)
            variance = jnp.mean(kept * kept, axis=1, keepdims=True)
            hn[part] = (kept * lax.rsqrt(variance + EPS) * hgain[...]).astype(BF16)

        tiles(step, 4)

    def clear_padding():
        pad = dn.shape[1] - ff

        def body(i, carry):
            dn[i, ff:] = jnp.zeros((pad, LANES), BF16)
            return carry

        if pad:
            lax.fori_loop(0, n, body, 0)

    sizes = {
        "half": half,
        "parts": parts,
        "row_bytes": [k.shape[2] * 2 for k in kinds],
        "hops": [[hops(kind, way) for way in range(2)] for kind in range(4)],
        "tok_bytes": rows * d * 2,
        "per": per,
        "chunk_bytes": rows * STEP_TILE * 2,
    }
    steps = {
        "z_own": z_own,
        "z_event": z_event,
        "y_start": y_start,
        "gather_start": lambda k: gather_start(x1_buf, k),
        "gather_on": lambda k: gather_on(x2_buf(k - 1) if k else x1_buf, k, rows),
        "gather_far": lambda k: gather_far(x2_buf(k - 1) if k else x1_buf, k, rows),
        "gather_mate": lambda k: gather_mate(x2_buf(k - 1) if k else x1_buf, k),
        "clear_padding": clear_padding,
        "make_decay": make_decay,
        "norm_tokens": norm_tokens,
        "gu_compute": gu_compute,
        "hidden": hidden,
        "project": lambda phase, s: project(3, s, hn, p2) if phase else project(1, s, hid, p1),
        "sum_start": sum_start,
        "sum_chip": sum_chip,
        "sum_on": sum_on,
        "after_first": after_first,
        "updated": updated,
        "qkv_compute": qkv_compute,
        "qkv_end": qkv_end,
        "retention": retention,
    }
    order = list(in_order(actions(sizes)))
    for i, (name, *args) in enumerate(order):
        if i == len(order) - 1:
            early, started[:] = started[:-8], started[-8:]
            for copy in early:
                copy.wait_send()
        with jax.named_scope(name):
            steps[name](*args)
    for copy in started:
        copy.wait_send()


def solution(mesh):
    n, n_tp, groups = mesh.shape["fs"], mesh.shape["tp"], mesh.shape["grp"]

    def shards(tokens, g1, g2, gate, up, down, query, key, value, head_gain, out, log_decay):
        rows, d = tokens.shape
        gate, up, log_decay = gate.T, up.T, log_decay.T
        ff = gate.shape[0]
        dk, dv = query.shape[1], value.shape[1]
        seq = rows * n_tp
        chunks = d // STEP_TILE
        ff_pad = -(-ff // LANES) * LANES
        vmem = pl.BlockSpec(memory_space=pltpu.VMEM)
        hbm = pl.BlockSpec(memory_space=pl.ANY)
        sums = [
            pltpu.VMEM((chunks, 2, n_tp // 2, rows, STEP_TILE), BF16),
            pltpu.VMEM((chunks, n_tp // 2, rows, STEP_TILE), BF16),
            pltpu.VMEM((chunks, n_tp // 2, rows, STEP_TILE), BF16),
            pltpu.VMEM((chunks, 2, rows // 2, STEP_TILE), BF16),
            pltpu.VMEM((chunks, 2, rows, STEP_TILE), BF16),
        ]
        dma = pltpu.SemaphoreType.DMA
        return pl.pallas_call(
            functools.partial(kernel, (n, groups)),
            out_shape=jax.ShapeDtypeStruct((rows, d), BF16),
            in_specs=[hbm, vmem, vmem, hbm, hbm, hbm, hbm, hbm, hbm, vmem, hbm, pl.BlockSpec(memory_space=pltpu.SMEM)],
            out_specs=vmem,
            scratch_shapes=[
                pltpu.VMEM((n, 2 * ff, LANES), BF16),
                pltpu.VMEM((n, ff_pad, LANES), BF16),
                pltpu.VMEM((n, LANES, 2 * dk + dv), BF16),
                pltpu.VMEM((n, dv, LANES), BF16),
                pltpu.VMEM((n_tp, rows, d), BF16),
                pltpu.VMEM((n, seq, LANES), BF16),
                pltpu.VMEM((seq, 2 * ff), F32),
                pltpu.VMEM((seq, ff_pad), BF16),
                *sums,
                pltpu.VMEM((chunks, n_tp, rows, STEP_TILE), BF16),
                *sums,
                pltpu.VMEM((seq, dk), BF16),
                pltpu.VMEM((seq, dk), BF16),
                pltpu.VMEM((seq, dv), BF16),
                pltpu.VMEM((seq, seq), F32),
                pltpu.VMEM((seq, dv), BF16),
                pltpu.VMEM((seq, LANES), F32),
                dma((8, 2, n // 2)),
                dma((8, 2, n // 2)),
                dma((4, 2, n // 2)),
                dma((4, 2, n // 2)),
                dma((2, chunks, 5)),
                dma((2, chunks, 5)),
                dma((1 + chunks, 8)),
                dma((1 + chunks, 8)),
                dma((10,)),
            ],
            compiler_params=pltpu.CompilerParams(
                collective_id=0, has_side_effects=True, vmem_limit_bytes=67_000_000
            ),
        )(
            tokens,
            g1.reshape(1, -1),
            g2.reshape(1, -1),
            gate,
            up,
            down,
            query,
            key,
            value,
            head_gain.reshape(1, -1),
            out,
            log_decay,
        )

    placed = (
        P(("grp", "fs", "tp"), None),
        P(),
        P(),
        P("fs", "tp"),
        P("fs", "tp"),
        P("tp", "fs"),
        P("fs", "tp"),
        P("fs", "tp"),
        P("fs", "tp"),
        P("tp"),
        P("tp", "fs"),
        P(None, "tp"),
    )
    return jax.shard_map(
        shards, mesh=mesh, in_specs=placed, out_specs=P(("grp", "fs", "tp"), None), check_vma=False
    )
```

```python
import functools

import jax
import jax.numpy as jnp
from jax import lax
from jax.experimental import pallas as pl
from jax.experimental.pallas import tpu as pltpu
from jax.sharding import PartitionSpec as P

EPS = 1e-06
MESH = pl.DeviceIdType.MESH
F32, BF16 = jnp.float32, jnp.bfloat16
LANES = 128
ROW_TILE = 16
STEP_TILE = 256
SHORTER = ((0, 1), (1, 0), (0, 1), (0, 1))
PAIR_SHARE = (0.376, 0.334, 0.25, 0.4)
PIECES = (3, 2, 3, 2)
RING_STARTS = ((((0, 1, 4),), ((0, 1, 5),)), (((1, 0, 3),), ((1, 0, 4),), ((1, 1, 4),)), (((2, 2, 4),), ((2, 0, 4),)))
RANKS = {'project': -3, 'qkv_compute': 2, 'gather_on': -1, 'gather_far': -12, 'gather_mate': -3, 'sum_start': -8, 'sum_chip': -1, 'sum_on': -4, 'after_first': 0, 'updated': -12, 'gu_compute': -2, 'out_start': -25, 'out_chip': -5, 'out_on': -1}
GU_TIME, KEEP_TIME, OUT_TIMES = 1.07, 0.8, (0.28, 0.47)
LINK, MATE = 46650.0, 600000.0
LATENCY = {"z0": 2.6, "z1": 2.6, "x0": 2.8, "x1": 2.8, "m": 1.0, "y": 3.0}


def split_rows(rows, share, pieces):
    pair = int(rows * share) // ROW_TILE
    units = rows // ROW_TILE - pair
    cuts = [-(-units * i // pieces) * ROW_TILE for i in range(pieces + 1)]
    return tuple(b - a for a, b in zip(cuts, cuts[1:])) + (pair * ROW_TILE,)


def actions(sizes):
    half, parts, row_bytes, hops = (sizes[k] for k in ("half", "parts", "row_bytes", "hops"))
    per, chunk = sizes["per"], sizes["chunk_bytes"]
    lasts = [per * (q + 1) for q in range(half // per)]
    acts = {}

    def act(name, rank, time, after=(), need=(), sends=()):
        acts[name] = (RANKS.get(name[0], rank), time, list(after), list(need), list(sends))

    def ways(kind, s):
        return [w for w in range(2) if s <= hops[kind][w]]

    def over_pair(kind, s):
        return [("y", kind, w, s) for w in ways(kind, s)]

    def landed(kind, s):
        return [("z_event", kind, sub, s) for sub in range(len(parts[kind]) - 1)]

    for kind in range(4):
        nbytes = [rows * row_bytes[kind] for rows in parts[kind]]
        subs = len(nbytes) - 1
        covered = min(sub for sub in range(subs) if sum(parts[kind][: sub + 1]) >= parts[kind][-1])
        for sub in range(subs):
            after = [("z_event", *v) for v in RING_STARTS[kind - 1][sub]] if kind else []
            own = [(f"z{w}", nbytes[sub], ("z", kind, sub, w, 1)) for w in range(2)]
            act(("z_own", kind, sub), -10 + 0.1 * kind, 0.03, after, (), own)
            for s in range(1, half + 1):
                need = [("z", kind, sub, w, s) for w in ways(kind, s)]
                onward = [(f"z{w}", nbytes[sub], ("z", kind, sub, w, s + 1)) for w in ways(kind, s + 1)]
                after = [("z_event", kind, sub, s - 1) if s > 1 else ("z_own", kind, sub)]
                act(("z_event", kind, sub, s), -20 + kind, 0.05, after, need, onward)
        for s in range(1, half + 1):
            after = [("z_event", kind, sub, s) for sub in range(covered + 1)]
            if s > 1 or kind:
                after.append(("y_start", kind, s - 1) if s > 1 else ("y_start", kind - 1, half))
            act(("y_start", kind, s), -15 + kind, 0.02, after, (), [("y", nbytes[-1], v) for v in over_pair(kind, s)])

    def gather(k, nbytes, first, rank):
        on = [("x0", nbytes / 2, 3), ("m", nbytes, 5), ("x1", nbytes / 2, 4), ("m", nbytes, 6)]
        for name, time, after, need, sends in (
            ("gather_on", 0.05, first, (0, 1), on),
            ("gather_far", 0.03, ("gather_on", k), (3, 4), [("m", nbytes, 7)]),
            ("gather_mate", 0.01, ("gather_far", k), (2, 5, 6, 7), []),
        ):
            tags = [("g", k, i) for i in need]
            act((name, k), rank, time, [after], tags, [(a, b, ("g", k, i)) for a, b, i in sends])
        return [(to, nbytes, ("g", k, i)) for i, to in enumerate(("x0", "x1", "m"))]

    sends = gather(0, sizes["tok_bytes"], ("gather_start", 0), -5)
    act(("gather_start", 0), -30, 0.06, (), (), sends)
    act(("clear_padding",), 50, 0.09)
    decays = [("make_decay", 2 * i, 2 * i + 2) for i in range(4)]
    for name in decays:
        act(name, 60, 0.36)
    norms = [("norm_tokens", 0, 4), ("norm_tokens", 4, 8)]
    for name in norms:
        act(name, -3, 0.92, [("gather_mate", 0)])
    for s in range(1, half + 1):
        after = landed(0, s) + (norms if s == 1 else [("gu_compute", s - 1)])
        act(("gu_compute", s), 0, GU_TIME, after, over_pair(0, s))
    act(("hidden",), 0, 0.85, [("gu_compute", half)])
    for q in range(len(lasts)):
        tag = [("s", 0, q, i) for i in range(5)]
        for s in range(lasts[q] - per + 1, lasts[q] + 1):
            after = landed(1, s) + [("project", s - 1) if s > 1 else ("hidden",), ("clear_padding",)]
            act(("project", s), 1, 0.75, after, over_pair(1, s))
        act(("sum_start", q), -4, 0.02, [("project", lasts[q])], (), [("m", 4 * chunk, tag[0])])
        sends = [("x0", chunk / 2, tag[1]), ("x1", chunk / 2, tag[2])]
        act(("sum_chip", q), -5, 0.16, [("sum_start", q)], tag[:1], sends)
        sends = [("x0", chunk, tag[3]), ("x1", chunk, tag[4])]
        act(("sum_on", q), -6, 0.06, [("sum_chip", q)], tag[1:3], sends)
        sends = gather(1 + q, chunk, ("after_first", q), -8)
        act(("after_first", q), -7, 0.14, [("sum_on", q)], tag[3:], sends)
    for m in range(4):
        act(("keep", m), 0 if m == 0 else 3, KEEP_TIME, [("keep", m - 1) if m else ("qkv_end",)] + decays)
    for m, time in enumerate(OUT_TIMES):
        for q in range(len(lasts)):
            tags = [("s", 1, q, 5 + i) for i in ((1, 2, 3) if m else (0,))]
            for s in range(lasts[q] - per + 1, lasts[q] + 1):
                after = landed(3, s) + [("out", s - 1, m) if s > 1 else ("keep", 3 * m)] + [("out", s, 0)] * m
                act(("out", s, m), 2 + 2 * m, time, after, over_pair(3, s))
            act(("out_start", q, m), -4, 0.03, [("out", lasts[q], m)], (), [("m", chunk, tag) for tag in tags])
            sends = [] if m else [("x0", chunk / 2, ("s", 1, q, 1)), ("x1", chunk / 2, ("s", 1, q, 2))]
            act(("out_chip", q, m), -5, 0.05, [("out_start", q, m)], tags, sends)
    for q in range(len(lasts)):
        tag = [("s", 1, q, i) for i in range(5)]
        sends = [("x0", chunk, tag[3]), ("x1", chunk, tag[4])]
        act(("out_on", q), -6, 0.06, [("out_chip", q, 0), ("out_chip", q, 1)], tag[1:3], sends)
        act(("updated", q), -1, 0.2, [("out_on", min(q + 4, len(lasts) - 1))], tag[3:])
    for s in range(1, half + 1):
        after = [("gather_mate", 1 + min(q for q, last in enumerate(lasts) if s <= last))] + landed(2, s)
        after.append(("qkv_compute", s - 1) if s > 1 else ("hidden",))
        act(("qkv_compute", s), 1.5, 0.92, after, over_pair(2, s))
    act(("qkv_end",), 0, 0.67, [("qkv_compute", half)])
    return acts


def in_order(acts, trace=None):
    arrival, free, done, left, now = {}, {}, set(), dict(acts), 0.0
    while left:
        ready = []
        for place, (name, (rank, _, after, need, _)) in enumerate(left.items()):
            if all(v in done for v in after) and all(v in arrival for v in need):
                ready.append((max([now] + [arrival[v] for v in need]), rank, place, name))
        begin, _, _, name = min(ready)
        _, time, _, _, sends = left.pop(name)
        if trace is not None:
            trace.append((name, now, begin))
        now = begin + time
        done.add(name)
        for link, nbytes, tag in sends:
            free[link] = max(free.get(link, 0.0), now) + nbytes / (MATE if link == "m" else LINK)
            arrival[tag] = free[link] + LATENCY[link]
        yield name


def half_mask(tile):
    return lax.broadcasted_iota(jnp.int32, tile.shape, 1) < LANES // 2


def kernel(
    sizes,
    tok_in,
    gain1,
    gain2,
    gate_in,
    up_in,
    down_in,
    q_in,
    k_in,
    v_in,
    hgain,
    out_in,
    rates,
    o_ref,
    gu,
    dn,
    qkv,
    wo,
    x1,
    x1n,
    acc,
    hid,
    p1,
    r1,
    s1,
    h1,
    f1,
    x2,
    p2,
    r2,
    s2,
    h2,
    f2,
    qs,
    ks,
    vs,
    decay,
    hn,
    ss,
    z_send,
    z_recv,
    y_send,
    y_recv,
    x_send,
    x_recv,
    a_send,
    a_recv,
    local_sem,
):
    n, groups = sizes
    half = n // 2
    d = n * LANES
    me = lax.axis_index("fs")
    r = lax.axis_index("tp")
    g = lax.axis_index("grp")
    up_z, down_z = lax.rem(me + 1, n), lax.rem(me + n - 1, n)
    x, c = r // 2, lax.rem(r, 2)
    xr, xl, xo = lax.rem(x + 1, 4), lax.rem(x + 3, 4), lax.rem(x + 2, 4)
    r_right, r_left, r_far = xr * 2 + c, xl * 2 + c, xo * 2 + c
    r_mate = x * 2 + 1 - c
    odd = lax.rem(g, 2)
    g_mate = g + 1 - 2 * odd
    rows = x1.shape[1]
    ff = gate_in.shape[0]
    main = ff // LANES * LANES
    started = []
    per = STEP_TILE // LANES // 2

    def remote(src, dst, ss_, rs_, **to):
        return pltpu.make_async_remote_copy(
            src_ref=src, dst_ref=dst, send_sem=ss_, recv_sem=rs_, device_id=to, device_id_type=MESH
        )

    def send(ref, dst, ss_, rs_, **to):
        copy = remote(ref, dst, ss_, rs_, **to)
        copy.start()
        started.append(copy)

    def arrived(ref, ss_, rs_, **to):
        remote(ref, ref, ss_, rs_, **to).wait_recv()

    local = []

    def fetch(src, dst):
        copy = pltpu.make_async_copy(src, dst, local_sem.at[len(local)])
        copy.start()
        local.append(copy)

    for i, weight in enumerate((gate_in, up_in)):
        fetch(weight.at[pl.ds(0, main)], gu.at[me, pl.ds(i * main, main)])
        fetch(weight.at[pl.ds(main, ff - main)], gu.at[me, pl.ds(2 * main + i * (ff - main), ff - main)])
    fetch(tok_in, x1.at[r])
    fetch(down_in, dn.at[me, pl.ds(0, ff)])
    dk, dv = q_in.shape[1], v_in.shape[1]
    fetch(q_in, qkv.at[me, :, pl.ds(0, dk)])
    fetch(k_in, qkv.at[me, :, pl.ds(dk, dk)])
    fetch(v_in, qkv.at[me, :, pl.ds(2 * dk, dv)])
    fetch(out_in, wo.at[me])

    barrier = pltpu.get_barrier_semaphore()
    neighbours = [
        {"fs": up_z},
        {"fs": down_z},
        {"tp": r_right},
        {"tp": r_left},
        {"tp": r_mate},
        {"grp": g_mate},
    ]
    for to in neighbours:
        pl.semaphore_signal(barrier, inc=1, device_id=to, device_id_type=MESH)
    with jax.named_scope("entry"):
        pl.semaphore_wait(barrier, len(neighbours))
    with jax.named_scope("fetched"):
        for copy in local:
            copy.wait()

    kinds = (gu, dn, qkv, wo)
    lengths = (gu.shape[1], ff, qkv.shape[1], wo.shape[1])
    parts = [split_rows(*v) for v in zip(lengths, PAIR_SHARE, PIECES)]

    def z_rows(kind, sub):
        size, start = parts[kind][sub], sum(parts[kind][:sub])
        mirrored = lengths[kind] - start - size
        return pl.ds(pl.multiple_of(start + odd * (mirrored - start), ROW_TILE), size)

    def y_rows(kind, sent):
        pair = parts[kind][-1]
        at = odd if sent else 1 - odd
        return pl.ds(pl.multiple_of(at * (lengths[kind] - pair), ROW_TILE), pair)

    def before(s):
        return lax.rem(me + n - s, n)

    def after(s):
        return lax.rem(me + s, n)

    def hops(kind, way):
        return half - SHORTER[kind][way]

    def z_start(kind, sub, way, s):
        block = before(s) if way == 0 else after(s)
        ref = kinds[kind].at[block, z_rows(kind, sub)]
        slot = (sum(PIECES[:kind]) + sub, way, s)
        send(ref, ref, z_send.at[slot], z_recv.at[slot], fs=up_z if way == 0 else down_z)

    def z_event(kind, sub, s):
        for way in range(2):
            if s > hops(kind, way):
                continue
            block = before(s) if way == 0 else after(s)
            ref = kinds[kind].at[block, z_rows(kind, sub)]
            slot = (sum(PIECES[:kind]) + sub, way, s - 1)
            arrived(ref, z_send.at[slot], z_recv.at[slot], fs=down_z if way == 0 else up_z)
            if s < hops(kind, way):
                z_start(kind, sub, way, s)
    def y_start(kind, s):
        for way in range(2):
            if s > hops(kind, way):
                continue
            block = before(s) if way == 0 else after(s)
            ref = kinds[kind].at[block, y_rows(kind, True)]
            slot = (kind, way, s - 1)
            send(ref, ref, y_send.at[slot], y_recv.at[slot], grp=g_mate)

    def z_own(kind, sub):
        for way in range(2):
            z_start(kind, sub, way, 0)

    def y_wait(kind, s):
        for way in range(2):
            if s > hops(kind, way):
                continue
            block = before(s) if way == 0 else after(s)
            ref = kinds[kind].at[block, y_rows(kind, False)]
            slot = (kind, way, s - 1)
            arrived(ref, y_send.at[slot], y_recv.at[slot], grp=g_mate)

    def pair_of(s):
        return (before(s), after(s)) if s < half else (me, after(half))

    def gather_start(buf, k):
        ref = buf(r)
        for i, to in enumerate((r_right, r_left, r_mate)):
            send(ref, ref, a_send.at[k, i], a_recv.at[k, i], tp=to)

    def gather_on(buf, k, count):
        for i, (src, onward) in enumerate(((r_left, r_right), (r_right, r_left))):
            ref = buf(src)
            arrived(ref, a_send.at[k, i], a_recv.at[k, i], tp=src)
            part = buf(src, pl.ds(i * (count // 2), count // 2))
            send(part, part, a_send.at[k, 3 + i], a_recv.at[k, 3 + i], tp=onward)
            send(ref, ref, a_send.at[k, 5 + i], a_recv.at[k, 5 + i], tp=r_mate)

    def gather_far(buf, k, count):
        for i, src in enumerate((r_left, r_right)):
            part = buf(r_far, pl.ds(i * (count // 2), count // 2))
            arrived(part, a_send.at[k, 3 + i], a_recv.at[k, 3 + i], tp=src)
        ref = buf(r_far)
        send(ref, ref, a_send.at[k, 7], a_recv.at[k, 7], tp=r_mate)

    def gather_mate(buf, k):
        for i, src in ((2, x), (5, xl), (6, xr), (7, xo)):
            ref = buf(src * 2 + 1 - c)
            arrived(ref, a_send.at[k, i], a_recv.at[k, i], tp=r_mate)

    def x1_buf(block, part=None):
        return x1.at[block] if part is None else x1.at[block, part]

    def x2_buf(q):
        def buf(block, part=None):
            return x2.at[q, block] if part is None else x2.at[q, block, part]

        return buf

    sides = ((r_left, r_right, xr), (r_right, r_left, xl))

    def on_mate(phase, q, i, to):
        p_, r_ = (p1, r1) if phase == 0 else (p2, r2)
        return p_.at[q, 1 - c, to], r_.at[q, to], x_send.at[phase, q, i], x_recv.at[phase, q, i]

    def add_mate(phase, q, to):
        p_, r_, s_ = (p1, r1, s1) if phase == 0 else (p2, r2, s2)
        s_[q, to] = (p_[q, c, to].astype(F32) + r_[q, to].astype(F32)).astype(BF16)

    def send_halves(phase, q):
        s_, h_ = (s1, h1) if phase == 0 else (s2, h2)
        for i, to in enumerate((r_right, r_left)):
            part = pl.ds(i * (rows // 2), rows // 2)
            send(s_.at[q, xo, part], h_.at[q, i], x_send.at[phase, q, 1 + i], x_recv.at[phase, q, 1 + i], tp=to)

    def sum_start(q):
        send(p1.at[q, 1 - c], r1.at[q], x_send.at[0, q, 0], x_recv.at[0, q, 0], tp=r_mate)

    def sum_chip(q):
        arrived(r1.at[q], x_send.at[0, q, 0], x_recv.at[0, q, 0], tp=r_mate)
        add_mate(0, q, xo)
        send_halves(0, q)
        for to in (xr, xl, x):
            add_mate(0, q, to)

    chips = (xo, xr, xl, x)

    def out_start(q, m):
        for i in (1, 2, 3) if m else (0,):
            src, dst, *sems = on_mate(1, q, 5 + i, chips[i])
            send(src, dst, *sems, tp=r_mate)

    def out_chip(q, m):
        for i in (1, 2, 3) if m else (0,):
            _, dst, *sems = on_mate(1, q, 5 + i, chips[i])
            arrived(dst, *sems, tp=r_mate)
            add_mate(1, q, chips[i])
        if m == 0:
            send_halves(1, q)

    def sum_on(phase, q):
        s_, h_, f_ = (s1, h1, f1) if phase == 0 else (s2, h2, f2)
        for i, (src, to, x_to) in enumerate(sides):
            arrived(h_.at[q, i], x_send.at[phase, q, 1 + i], x_recv.at[phase, q, 1 + i], tp=src)
            part = pl.ds(i * (rows // 2), rows // 2)
            s_[q, x_to, part] = (s_[q, x_to, part].astype(F32) + h_[q, i].astype(F32)).astype(BF16)
            send(s_.at[q, x_to], f_.at[q, i], x_send.at[phase, q, 3 + i], x_recv.at[phase, q, 3 + i], tp=to)

    def sum_end(phase, q):
        s_, f_ = (s1, f1) if phase == 0 else (s2, f2)
        for i, src in enumerate((r_left, r_right)):
            arrived(f_.at[q, i], x_send.at[phase, q, 3 + i], x_recv.at[phase, q, 3 + i], tp=src)
        return s_[q, x].astype(F32) + f_[q, 0].astype(F32) + f_[q, 1].astype(F32)

    def block_lanes(block):
        return pl.ds(pl.multiple_of(block * LANES, LANES), LANES)

    def blocks_of(q):
        return [b for s in range(q * per + 1, (q + 1) * per + 1) for b in pair_of(s)]

    def after_first(q):
        total = sum_end(0, q)
        for i, block in enumerate(blocks_of(q)):
            cols = slice(i * LANES, (i + 1) * LANES)
            base = x1[r, :, block_lanes(block)].astype(F32)
            x2[q, r, :, cols] = (base + 0.5 * total[:, cols]).astype(BF16)
        gather_start(x2_buf(q), 1 + q)

    def updated(q):
        total = sum_end(1, q) + x2[q, r].astype(F32)
        for i, block in enumerate(blocks_of(q)):
            o_ref[:, block_lanes(block)] = total[:, i * LANES : (i + 1) * LANES].astype(BF16)

    seq = x1n.shape[1]
    tile = seq // 2

    def norm_tokens(first, last):
        def body(i, carry):
            value = x1[i].astype(F32)
            factor = lax.rsqrt(jnp.mean(value * value, axis=1, keepdims=True) + EPS)
            value = (value * factor * gain1[...]).astype(BF16)
            to = pl.ds(pl.multiple_of(i * rows, rows), rows)
            for b in range(n):
                x1n[b, to] = value[:, b * LANES : (b + 1) * LANES]
            return carry

        lax.fori_loop(first, last, body, 0)

    def tiles(step, count=2):
        def body(m, carry):
            step(m)
            return carry

        lax.fori_loop(0, count, body, 0)

    def gu_compute(s):
        y_wait(0, s)
        a, b = pair_of(s)

        def step(m):
            part = pl.ds(pl.multiple_of(m * tile, tile), tile)
            left = jnp.concatenate([x1n[a, part], x1n[b, part]], axis=1)
            right = jnp.concatenate([gu[a], gu[b]], axis=1)
            product = lax.dot_general(left, right, (((1,), (1,)), ((), ())), preferred_element_type=F32)
            acc[part] = product if s == 1 else acc[part] + product

        tiles(step)

    def silu_times(gate, up_value):
        return gate / (1.0 + jnp.exp(-gate)) * up_value

    def hidden():
        size = seq // 8

        def step(m):
            part = pl.ds(pl.multiple_of(m * size, size), size)
            hid[part, :main] = silu_times(acc[part, :main], acc[part, main : 2 * main]).astype(BF16)
            last = acc[part, 2 * main :]
            value = silu_times(last, pltpu.roll(last, LANES // 2, 1))
            hid[part, main:] = jnp.where(half_mask(value), value, 0.0).astype(BF16)

        tiles(step, 8)

    def project(s):
        y_wait(1, s)
        a, b = pair_of(s)
        q, at = (s - 1) // per, (s - 1) % per * 2 * LANES

        def step(m):
            part = pl.ds(pl.multiple_of(m * tile, tile), tile)
            right = jnp.concatenate([dn[a], dn[b]], axis=1)
            product = jnp.dot(hid[part], right, preferred_element_type=F32).astype(BF16)
            for i in range(tile // rows):
                to = m * (tile // rows // 2) + i // 2
                p1[q, i % 2, to, :, at : at + 2 * LANES] = product[i * rows : (i + 1) * rows]

        tiles(step)

    def out(s, m):
        if m == 0:
            y_wait(3, s)
        a, b = pair_of(s)
        q, at = (s - 1) // per, (s - 1) % per * 2 * LANES
        first, last = (1, 4) if m else (0, 1)
        left = hn[first * 2 * rows : last * 2 * rows]
        right = jnp.concatenate([wo[a], wo[b]], axis=1)
        product = jnp.dot(left, right, preferred_element_type=F32).astype(BF16)
        for i in range(2 * (last - first)):
            p2[q, i % 2, chips[first + i // 2], :, at : at + 2 * LANES] = product[i * rows : (i + 1) * rows]

    def qkv_compute(s):
        y_wait(2, s)
        a, b = pair_of(s)
        q, at = (s - 1) // per, (s - 1) % per * 2 * LANES
        gain = jnp.concatenate([gain2[:, block_lanes(a)], gain2[:, block_lanes(b)]], axis=1)
        count = tile // rows
        width = qkv.shape[2]

        def step(m):
            part = pl.ds(pl.multiple_of(m * tile, tile), tile)
            value = x2[q, pl.ds(m * count, count), :, at : at + 2 * LANES].reshape(tile, 2 * LANES).astype(F32)
            square = value * value
            square = square[:, :LANES] + square[:, LANES:]
            right = jnp.concatenate([qkv[a], qkv[b]], axis=0)
            product = jnp.dot((value * gain).astype(BF16), right, preferred_element_type=F32)
            acc[part, :width] = product if s == 1 else acc[part, :width] + product
            ss[part] = square if s == 1 else ss[part] + square

        tiles(step)

    def qkv_end():
        size = seq // 4
        scale = dk**-0.5

        def step(m):
            part = pl.ds(pl.multiple_of(m * size, size), size)
            factor = lax.rsqrt(jnp.sum(ss[part], axis=1, keepdims=True) / d + EPS)
            qs[part] = ((acc[part, :dk] * factor).astype(BF16).astype(F32) * scale).astype(BF16)
            ks[part] = (acc[part, dk : 2 * dk] * factor).astype(BF16)
            vs[part] = (acc[part, 2 * dk : 2 * dk + dv] * factor).astype(BF16)

        tiles(step, 4)

    def make_decay(first, last):
        size = seq // 8
        forward, backward = rates[0, 0], rates[0, 1]

        def body(m, carry):
            at = lax.broadcasted_iota(jnp.int32, (size, seq), 0) + m * size
            gap = at - lax.broadcasted_iota(jnp.int32, (size, seq), 1)
            far = gap.astype(F32)
            weight = jnp.exp(jnp.where(gap >= 0, forward * far, -backward * far))
            decay[pl.ds(pl.multiple_of(m * size, size), size)] = jnp.where(gap == 0, 2.0, weight)
            return carry

        lax.fori_loop(first, last, body, 0)

    def keep(m):
        part = pl.ds(pl.multiple_of(chips[m] * 2 * rows, 2 * rows), 2 * rows)
        score = lax.dot_general(qs[part], ks[...], (((1,), (1,)), ((), ())), preferred_element_type=F32)
        kept = jnp.dot((score * decay[part]).astype(BF16), vs[...], preferred_element_type=F32)
        kept = kept - jnp.mean(kept, axis=1, keepdims=True)
        variance = jnp.mean(kept * kept, axis=1, keepdims=True)
        hn[m * 2 * rows : (m + 1) * 2 * rows] = (kept * lax.rsqrt(variance + EPS) * hgain[...]).astype(BF16)

    def clear_padding():
        pad = dn.shape[1] - ff

        def body(i, carry):
            dn[i, ff:] = jnp.zeros((pad, LANES), BF16)
            return carry

        if pad:
            lax.fori_loop(0, n, body, 0)

    sizes = {
        "half": half,
        "parts": parts,
        "row_bytes": [k.shape[2] * 2 for k in kinds],
        "hops": [[hops(kind, way) for way in range(2)] for kind in range(4)],
        "tok_bytes": rows * d * 2,
        "per": per,
        "chunk_bytes": rows * STEP_TILE * 2,
    }
    steps = {
        "z_own": z_own,
        "z_event": z_event,
        "y_start": y_start,
        "gather_start": lambda k: gather_start(x1_buf, k),
        "gather_on": lambda k: gather_on(x2_buf(k - 1) if k else x1_buf, k, rows),
        "gather_far": lambda k: gather_far(x2_buf(k - 1) if k else x1_buf, k, rows),
        "gather_mate": lambda k: gather_mate(x2_buf(k - 1) if k else x1_buf, k),
        "clear_padding": clear_padding,
        "make_decay": make_decay,
        "norm_tokens": norm_tokens,
        "gu_compute": gu_compute,
        "hidden": hidden,
        "project": project,
        "sum_start": sum_start,
        "sum_chip": sum_chip,
        "sum_on": lambda q: sum_on(0, q),
        "keep": keep,
        "out": out,
        "out_start": out_start,
        "out_chip": out_chip,
        "out_on": lambda q: sum_on(1, q),
        "after_first": after_first,
        "updated": updated,
        "qkv_compute": qkv_compute,
        "qkv_end": qkv_end,
    }
    order = list(in_order(actions(sizes)))
    for i, (name, *args) in enumerate(order):
        if i == len(order) - 1:
            early, started[:] = started[:-8], started[-8:]
            for copy in early:
                copy.wait_send()
        with jax.named_scope(name):
            steps[name](*args)
    for copy in started:
        copy.wait_send()


def solution(mesh):
    n, n_tp, groups = mesh.shape["fs"], mesh.shape["tp"], mesh.shape["grp"]

    def shards(tokens, g1, g2, gate, up, down, query, key, value, head_gain, out, log_decay):
        rows, d = tokens.shape
        gate, up, log_decay = gate.T, up.T, log_decay.T
        ff = gate.shape[0]
        dk, dv = query.shape[1], value.shape[1]
        seq = rows * n_tp
        chunks = d // STEP_TILE
        ff_pad = -(-ff // LANES) * LANES
        vmem = pl.BlockSpec(memory_space=pltpu.VMEM)
        hbm = pl.BlockSpec(memory_space=pl.ANY)
        sums = [
            pltpu.VMEM((chunks, 2, n_tp // 2, rows, STEP_TILE), BF16),
            pltpu.VMEM((chunks, n_tp // 2, rows, STEP_TILE), BF16),
            pltpu.VMEM((chunks, n_tp // 2, rows, STEP_TILE), BF16),
            pltpu.VMEM((chunks, 2, rows // 2, STEP_TILE), BF16),
            pltpu.VMEM((chunks, 2, rows, STEP_TILE), BF16),
        ]
        dma = pltpu.SemaphoreType.DMA
        return pl.pallas_call(
            functools.partial(kernel, (n, groups)),
            out_shape=jax.ShapeDtypeStruct((rows, d), BF16),
            in_specs=[hbm, vmem, vmem, hbm, hbm, hbm, hbm, hbm, hbm, vmem, hbm, pl.BlockSpec(memory_space=pltpu.SMEM)],
            out_specs=vmem,
            scratch_shapes=[
                pltpu.VMEM((n, 2 * ff, LANES), BF16),
                pltpu.VMEM((n, ff_pad, LANES), BF16),
                pltpu.VMEM((n, LANES, 2 * dk + dv), BF16),
                pltpu.VMEM((n, dv, LANES), BF16),
                pltpu.VMEM((n_tp, rows, d), BF16),
                pltpu.VMEM((n, seq, LANES), BF16),
                pltpu.VMEM((seq, 2 * ff), F32),
                pltpu.VMEM((seq, ff_pad), BF16),
                *sums,
                pltpu.VMEM((chunks, n_tp, rows, STEP_TILE), BF16),
                *sums,
                pltpu.VMEM((seq, dk), BF16),
                pltpu.VMEM((seq, dk), BF16),
                pltpu.VMEM((seq, dv), BF16),
                pltpu.VMEM((seq, seq), F32),
                pltpu.VMEM((seq, dv), BF16),
                pltpu.VMEM((seq, LANES), F32),
                dma((sum(PIECES), 2, n // 2)),
                dma((sum(PIECES), 2, n // 2)),
                dma((4, 2, n // 2)),
                dma((4, 2, n // 2)),
                dma((2, chunks, 9)),
                dma((2, chunks, 9)),
                dma((1 + chunks, 8)),
                dma((1 + chunks, 8)),
                dma((10,)),
            ],
            compiler_params=pltpu.CompilerParams(
                collective_id=0, has_side_effects=True, vmem_limit_bytes=67_000_000
            ),
        )(
            tokens,
            g1.reshape(1, -1),
            g2.reshape(1, -1),
            gate,
            up,
            down,
            query,
            key,
            value,
            head_gain.reshape(1, -1),
            out,
            log_decay,
        )

    placed = (
        P(("grp", "fs", "tp"), None),
        P(),
        P(),
        P("fs", "tp"),
        P("fs", "tp"),
        P("tp", "fs"),
        P("fs", "tp"),
        P("fs", "tp"),
        P("fs", "tp"),
        P("tp"),
        P("tp", "fs"),
        P(None, "tp"),
    )
    return jax.shard_map(
        shards, mesh=mesh, in_specs=placed, out_specs=P(("grp", "fs", "tp"), None), check_vma=False
    )
```
